32 devices in a mesh: grp: 2 (over x), ep: 4 (over y, core), tp: 4 (over z).
Axes of the slice: x: 2, y: 2, z: 4, core: 2. Of those that a mesh axis runs over, the one named last changes fastest.
Arguments:
- queries: bfloat16 [2048, 2048], P(('grp', 'ep'), 'tp'), parts along dimension 0, may hold values from -6 to 6
- key_rows: bfloat16 [2048, 2048], P(('grp', 'ep'), 'tp'), parts along dimension 0, may hold values from -6 to 6
- values: bfloat16 [2048, 4096], P(('grp', 'ep'), 'tp'), parts along dimension 0, may hold values from -6 to 6
- log_decay: float32 [8, 1024], P('tp', 'ep'), may hold values from -1 to 0
- out_weight: bfloat16 [4096, 2048], P('tp'), may hold values from -0.09375 to 0.09375
- expert_input: bfloat16 [4096, 2048], P(('grp', 'ep')), parts along dimension 0, may hold values from -6 to 6
- expert_gain: float32 [2048], replicated, may hold values from 0.1 to 1.9
- route_ids: int32 [4096, 2], P(('grp', 'ep')), parts along dimension 0, may hold values from 0 to 3, all different within a row; in each aligned block of 128 rows (0 to 127, 128 to 255, ...) at most 72 rows name the same one
- route_weights: float32 [4096, 2], P(('grp', 'ep')), parts along dimension 0, may hold values from 0.2 to 1
- gate_weight: bfloat16 [4, 2048, 3584], P('ep', None, 'tp'), may hold values from -0.125 to 0.125
- up_weight: bfloat16 [4, 2048, 3584], P('ep', None, 'tp'), may hold values from -0.125 to 0.125
- down_weight: bfloat16 [4, 3584, 2048], P('ep', 'tp'), may hold values from -0.09375 to 0.09375
Outputs:
- mixer_out: bfloat16 [2048, 2048], P(('grp', 'ep', 'tp')), parts along dimension 0
- expert_out: bfloat16 [4096, 2048], P(('grp', 'ep', 'tp')), parts along dimension 0
The draws below stay inside these ranges and needn't reach their ends.
There are 2 independent parts, one for each index of `grp`. The reference program is written for one: setup_inputs(seed, part) draws one part's arguments, and reference() takes and returns one part's arrays. A program takes and returns all parts, laid end to end along the dimension named above; an argument that names none is the same for every part. Nothing has to cross between parts.
Inputs may be any that keep to these rules, and one draw needn't show every extreme that they name: `route_ids`: each row names 2 different experts; within each aligned block of 128 rows no expert is named more than 72 times, a bound that some block reaches.
All inputs are finite; a program needn't handle non-finite values.
Results may differ from the reference program's by a relative error of at most 0.02.
Values may be sent and summed in bfloat16 or wider, within the bound.
A program may use at most 128 MiB of HBM per device.

```python
import math
import jax
import jax.numpy as jnp
import numpy as np
from jax import lax

D = 2048
RETENTION_HEADS = 8
DK = 256
DV = 512
FE = 3584
TOP = 2
BLOCK = 256
TOK_DEV = 128
SEQUENCE_LENGTH = 1024
EXPERTS = 4
TOKENS = 2048
CAP_T = 72
N_TP = 4


def draw_log_decay(key, part):
    random_sources = jax.random.split(jax.random.fold_in(key, 17), 7)
    fast_share = 0.5
    fast_head = jax.random.uniform(random_sources[0], (RETENTION_HEADS,), jnp.float32) < fast_share
    fast_rate = jnp.exp(jax.random.uniform(random_sources[1], (RETENTION_HEADS,), jnp.float32, jnp.log(1.0 / 100.0), jnp.log(1.0 / 30.0)))
    slow_rate = jax.random.uniform(random_sources[2], (RETENTION_HEADS,), jnp.float32, 0.05, 0.3) / SEQUENCE_LENGTH
    baseline_decay_rate = jnp.where(fast_head, fast_rate, slow_rate)
    block_count = SEQUENCE_LENGTH // BLOCK
    block_multiplier = jnp.exp(jax.random.uniform(random_sources[3], (RETENTION_HEADS, block_count), jnp.float32, jnp.log(0.5), jnp.log(2.0)))
    block_multiplier = jnp.repeat(block_multiplier, BLOCK, axis=1)
    decay_jitter = jax.random.uniform(random_sources[4], (RETENTION_HEADS, SEQUENCE_LENGTH), jnp.float32, 0.5, 1.5)
    spike_location = jax.random.randint(random_sources[5], (RETENTION_HEADS, 2), 0, SEQUENCE_LENGTH)
    spike_length = jnp.log(jax.random.uniform(random_sources[6], (RETENTION_HEADS, 2), jnp.float32, 0.6, 0.8))
    position_indices = jnp.arange(SEQUENCE_LENGTH, dtype=jnp.int32)
    decay_spikes = jnp.sum(jnp.where(position_indices[None, None, :] == spike_location[:, :, None], spike_length[:, :, None], 0.0), axis=1)
    return (-baseline_decay_rate[:, None] * block_multiplier * decay_jitter + decay_spikes).astype(jnp.float32)


def level_of(own_key, extent, cuts, smallest, high):
    factor_of = 1.0
    for axis_at, blocks in cuts:
        heights = jax.random.uniform(jax.random.fold_in(jax.random.fold_in(own_key, 6), axis_at), (blocks,), jnp.float32, smallest / len(cuts), high / len(cuts))
        factor_of = factor_of * jnp.repeat(jnp.exp(heights), extent[axis_at] // blocks).reshape((-1,) + (1,) * (len(extent) - 1 - axis_at))
    return factor_of


def assign_block(stream_key, own, number, rows, count, top, most, slope):
    sequence = jax.random.permutation(stream_key, count)
    packed, usual = portions_of(count, rows * top, most, slope, True), portions_of(count, rows * top, most, slope, False)
    places = jnp.arange(count)

    def named(lengths, turn):
        used = int((lengths > 0).sum())
        fixed = max(1, used // 4)
        passed = fixed + (places - fixed + turn * (used - fixed)) % max(1, count - fixed)
        return jnp.zeros((count,), jnp.int32).at[sequence[jnp.where(places < fixed, places, passed)]].set(jnp.asarray(lengths, jnp.int32))

    lengths = jnp.where(number % 4 == 0, named(packed, number // 4), named(usual, number - number // 4 - 1))
    mixed = jax.random.permutation(jax.random.fold_in(own, 3), count)
    donor, sink = mixed[0:count // 2 * 2:2], mixed[1:count // 2 * 2:2]
    room = jnp.minimum(lengths[donor] - 1, most - lengths[sink]) // 2
    room = jnp.where((donor == sequence[0]) | (sink == sequence[0]) | (lengths[sink] == 0), 0, jnp.maximum(room, 0))
    passed = jax.random.randint(jax.random.fold_in(own, 4), (count // 2,), 0, 1 << 20) % (room + 1)
    lengths = lengths.at[donor].add(-passed).at[sink].add(passed)
    labels = jnp.searchsorted(jnp.cumsum(lengths), jnp.arange(rows * top), side="right").astype(jnp.int32)
    grid = labels.reshape(top, rows).T
    grid = grid[jax.random.permutation(jax.random.fold_in(own, 1), rows)]
    turn = jax.random.randint(jax.random.fold_in(own, 2), (rows, 1), 0, top)
    return jnp.take_along_axis(grid, (jnp.arange(top)[None, :] + turn) % top, axis=1)


def portions_of(amount, total, reach, slope, full):
    portions = [(1 << 20) // math.isqrt(rank ** slope) + 1 for rank in range(1, amount + 1)]
    largest = reach if full else min(reach, max(-(-total // amount), total * portions[0] // sum(portions)))
    least = 1 if total - largest >= amount - 1 else 0
    given, surplus = [largest] + [least] * (amount - 1), total - largest - least * (amount - 1)
    while surplus > 0:
        candidates = [i for i in range(1, amount) if given[i] < largest] or [i for i in range(1, amount) if given[i] < reach]
        mass, budget = sum([portions[i] for i in candidates]), surplus
        for i in candidates:
            addition = min(reach - given[i], max(1, budget * portions[i] // mass), surplus)
            given[i] = given[i] + addition
            surplus = surplus - addition
    return np.array(given)


def bell_draw(rng, dims, scale, most, shards=(), held_as=jnp.bfloat16):
    level = level_of(rng, dims, shards, -0.22, 0.18) if shards else 1.0
    values = jax.random.normal(rng, dims, jnp.float32) * scale * level
    return jnp.minimum(jnp.maximum(values, -most), most).astype(held_as)


def setup_inputs(seed: int = 0, part: int = 0) -> dict:
    streams_of = jax.random.split(jax.random.key(seed), 13)
    part_splits = jax.random.split(jax.random.fold_in(streams_of[12], part), 13)
    queries = bell_draw(part_splits[0], (SEQUENCE_LENGTH, RETENTION_HEADS * DK), 1.0, 6.0, ((0, 4), (1, 4)))
    key_rows = bell_draw(part_splits[1], (SEQUENCE_LENGTH, RETENTION_HEADS * DK), 1.0, 6.0, ((0, 4), (1, 4)))
    values = bell_draw(part_splits[2], (SEQUENCE_LENGTH, RETENTION_HEADS * DV), 1.0, 6.0, ((0, 4), (1, 4)))
    log_decay = draw_log_decay(jax.random.fold_in(streams_of[12], 71), part)
    out_weight = bell_draw(streams_of[4], (RETENTION_HEADS * DV, D), (RETENTION_HEADS * DV) ** -0.5, 0.09375, ((0, 4),))
    expert_input = bell_draw(part_splits[5], (TOKENS, D), 1.0, 6.0, ((0, 4),))
    expert_gain = jnp.clip(1.0 + 0.18 * jax.random.normal(streams_of[6], (D,), jnp.float32), 0.1, 1.9)
    route_ids_keys = jax.random.split(jax.random.fold_in(part_splits[7], 1), TOKENS // TOK_DEV)
    route_ids_turns = jax.random.permutation(jax.random.fold_in(part_splits[7], 3), TOKENS // TOK_DEV)
    route_ids = jax.vmap(lambda own, number: assign_block(jax.random.fold_in(part_splits[7], 2), own, number, TOK_DEV, EXPERTS, TOP, CAP_T, 0))(route_ids_keys, route_ids_turns).reshape((TOKENS, TOP))
    route_weights = jnp.clip(0.2 + 0.8 * jax.random.uniform(part_splits[8], (TOKENS, TOP), jnp.float32) ** level_of(part_splits[8], (TOKENS, TOP), ((0, 4),), -0.2, 0.2), 0.2, 1.0)
    gate_weight = bell_draw(streams_of[9], (EXPERTS, D, FE), D ** -0.5, 0.125, ((0, 4), (2, 4)))
    up_weight = bell_draw(streams_of[10], (EXPERTS, D, FE), D ** -0.5, 0.125, ((0, 4), (2, 4)))
    down_weight = bell_draw(streams_of[11], (EXPERTS, FE, D), FE ** -0.5, 0.09375, ((0, 4), (1, 4)))
    return dict(queries=queries, key_rows=key_rows, values=values, log_decay=log_decay, out_weight=out_weight, expert_input=expert_input, expert_gain=expert_gain, route_ids=route_ids, route_weights=route_weights, gate_weight=gate_weight, up_weight=up_weight, down_weight=down_weight)


epsilon = 1e-06
rope_base = 10000.0

def rounded(tensor):
    return lax.optimization_barrier(tensor.astype(jnp.bfloat16)).astype(jnp.float32)

def rotate(tensor, position_indices):
    width = tensor.shape[-1]
    middle = width // 2
    inverse = rope_base ** (-jnp.arange(0, width, 2, dtype=jnp.float32) / width)
    angles = position_indices.astype(jnp.float32)[:, None] * inverse[None, :]
    cosine = jnp.cos(angles)[:, None, :]
    sine_part = jnp.sin(angles)[:, None, :]
    first_half = tensor[..., :middle]
    second_half = tensor[..., middle:]
    return jnp.concatenate([first_half * cosine - second_half * sine_part, second_half * cosine + first_half * sine_part], axis=-1)

def retention_part(queries, key_rows, values, log_decay, out_weight):
    length = queries.shape[0]
    position_indices = jnp.arange(length, dtype=jnp.int32)
    rotated_q = rotate(queries.astype(jnp.float32).reshape(length, RETENTION_HEADS, DK), position_indices).astype(jnp.bfloat16)
    rotated_k = (rotate(key_rows.astype(jnp.float32).reshape(length, RETENTION_HEADS, DK), position_indices) * DK ** (-0.5)).astype(jnp.bfloat16)
    value_rows = values.reshape(length, RETENTION_HEADS, DV)
    blocks = length // BLOCK
    query_blocks = rotated_q.reshape(blocks, BLOCK, RETENTION_HEADS, DK)
    key_blocks = rotated_k.reshape(blocks, BLOCK, RETENTION_HEADS, DK)
    value_blocks = value_rows.reshape(blocks, BLOCK, RETENTION_HEADS, DV)
    rate_blocks = log_decay.reshape(RETENTION_HEADS, blocks, BLOCK).transpose(1, 0, 2)
    lane = jnp.arange(BLOCK, dtype=jnp.int32)
    causal = lane[:, None] >= lane[None, :]

    def advance(carried, inputs):
        query_now, key_now, value_now, rates = inputs
        cumulative = jnp.cumsum(rates, axis=-1)
        block_end = cumulative[:, -1:]
        spread = cumulative[:, :, None] - cumulative[:, None, :]
        weight = jnp.where(causal[None], jnp.exp(jnp.minimum(spread, 0.0)), 0.0)
        scores = jnp.einsum('thd,shd->hts', query_now.astype(jnp.float32), key_now.astype(jnp.float32)) * weight
        within = jnp.einsum('hts,she->the', rounded(scores), value_now.astype(jnp.float32))
        carried_part = jnp.einsum('thd,hde->the', query_now.astype(jnp.float32), rounded(carried))
        carried_part = carried_part * jnp.exp(cumulative).T[:, :, None]
        weighted_k = rounded(key_now.astype(jnp.float32) * jnp.exp(block_end - cumulative).T[:, :, None])
        carried = carried * jnp.exp(block_end)[:, :, None] + jnp.einsum('thd,the->hde', weighted_k, value_now.astype(jnp.float32))
        return (carried, within + carried_part)
    start_state = jnp.zeros((RETENTION_HEADS, DK, DV), jnp.float32)
    _, outputs = lax.scan(advance, start_state, (query_blocks, key_blocks, value_blocks, rate_blocks))
    result = outputs.reshape(length, RETENTION_HEADS, DV)
    center = lax.optimization_barrier(jnp.mean(result, axis=-1, keepdims=True))
    variance = lax.optimization_barrier(jnp.mean(jnp.square(result - center), axis=-1, keepdims=True))
    normed = ((result - center) * lax.rsqrt(variance + epsilon)).astype(jnp.bfloat16).reshape(length, RETENTION_HEADS * DV)
    group_width = RETENTION_HEADS * DV // N_TP
    summed = jnp.zeros((length, D), jnp.float32)
    for group in range(N_TP):
        partial_value = jnp.dot(normed[:, group * group_width:(group + 1) * group_width], out_weight[group * group_width:(group + 1) * group_width], preferred_element_type=jnp.float32)
        summed = summed + rounded(partial_value)
    return summed.astype(jnp.bfloat16)

def expert_part(expert_input, expert_gain, route_ids, route_weights, gate_weight, up_weight, down_weight):
    count_tokens = expert_input.shape[0]
    count_experts = gate_weight.shape[0]
    choose = route_ids.shape[1]
    widened = expert_input.astype(jnp.float32)
    normed = (widened * lax.rsqrt(lax.optimization_barrier(jnp.mean(widened * widened, axis=-1, keepdims=True)) + epsilon) * expert_gain).astype(jnp.bfloat16)
    block_count = count_tokens // TOK_DEV
    flat_routes = route_ids.reshape(block_count, TOK_DEV * choose)
    onehot = (flat_routes[:, :, None] == jnp.arange(count_experts, dtype=jnp.int32)[None, None, :]).astype(jnp.int32)
    ranks = (lax.optimization_barrier(jnp.sum(jnp.cumsum(onehot, axis=1) * onehot, axis=-1)) - 1).reshape(count_tokens, choose)
    block_of = (jnp.arange(count_tokens, dtype=jnp.int32) // TOK_DEV)[:, None]
    slot_index = (block_of * CAP_T + ranks).astype(jnp.int32)
    token_index = jnp.broadcast_to(jnp.arange(count_tokens, dtype=jnp.int32)[:, None], (count_tokens, choose))
    slot_token = jnp.zeros((count_experts, block_count * CAP_T), jnp.int32).at[route_ids, slot_index].set(token_index)
    filled = jnp.zeros((count_experts, block_count * CAP_T), jnp.float32).at[route_ids, slot_index].set(1.0)
    group_width = FE // N_TP

    def one_expert(inputs):
        table, present, gate_one, up_one, down_one = inputs
        gathered = normed[table] * present[:, None].astype(jnp.bfloat16)
        gate_part = jnp.dot(gathered, gate_one, preferred_element_type=jnp.float32)
        up_part = jnp.dot(gathered, up_one, preferred_element_type=jnp.float32)
        hidden = (jax.nn.silu(gate_part) * up_part).astype(jnp.bfloat16)
        summed = jnp.zeros((table.shape[0], D), jnp.float32)
        for group in range(N_TP):
            partial_value = jnp.dot(hidden[:, group * group_width:(group + 1) * group_width], down_one[group * group_width:(group + 1) * group_width], preferred_element_type=jnp.float32)
            summed = summed + rounded(partial_value)
        return summed.astype(jnp.bfloat16)
    outputs = lax.map(one_expert, (slot_token, filled, gate_weight, up_weight, down_weight))
    picked = outputs[route_ids, slot_index]
    combined = lax.optimization_barrier(jnp.sum(picked.astype(jnp.float32) * route_weights[:, :, None], axis=1))
    return combined.astype(jnp.bfloat16)

def reference(queries, key_rows, values, log_decay, out_weight, expert_input, expert_gain, route_ids, route_weights, gate_weight, up_weight, down_weight):
    mixer_out = retention_part(queries, key_rows, values, log_decay, out_weight)
    expert_out = expert_part(expert_input, expert_gain, route_ids, route_weights, gate_weight, up_weight, down_weight)
    return (mixer_out, expert_out)
```

```python
import jax
import jax.numpy as jnp
from jax import lax
from jax.sharding import PartitionSpec as P

BLOCK = 256


epsilon = 1e-06
rope_base = 10000.0


def rotate(tensor, position_indices):
    width = tensor.shape[-1]
    middle = width // 2
    inverse = rope_base ** (-jnp.arange(0, width, 2, dtype=jnp.float32) / width)
    angles = position_indices.astype(jnp.float32)[:, None] * inverse[None, :]
    cosine = jnp.cos(angles)[:, None, :]
    sine_part = jnp.sin(angles)[:, None, :]
    first_half = tensor[..., :middle]
    second_half = tensor[..., middle:]
    return jnp.concatenate(
        [
            first_half * cosine - second_half * sine_part,
            second_half * cosine + first_half * sine_part,
        ],
        axis=-1,
    )


def retention_part(queries, key_rows, values, log_decay, out_weight):
    seq_rows = queries.shape[0]
    local_heads = log_decay.shape[0]
    key_width = queries.shape[1] // local_heads
    value_width = values.shape[1] // local_heads
    blocks = seq_rows // BLOCK
    position_indices = lax.axis_index("ep") * seq_rows + jnp.arange(seq_rows, dtype=jnp.int32)
    rotated_q = rotate(
        queries.astype(jnp.float32).reshape(seq_rows, local_heads, key_width), position_indices
    )
    rotated_q = rotated_q.astype(jnp.bfloat16).reshape(blocks, BLOCK, local_heads, key_width)
    rotated_k = rotate(
        key_rows.astype(jnp.float32).reshape(seq_rows, local_heads, key_width), position_indices
    ) * key_width ** (-0.5)
    rotated_k = rotated_k.astype(jnp.bfloat16).reshape(blocks, BLOCK, local_heads, key_width)
    value_blocks = values.reshape(blocks, BLOCK, local_heads, value_width)
    cumulative = jnp.cumsum(log_decay.reshape(local_heads, blocks, BLOCK), axis=-1)
    block_end = cumulative[:, :, -1]
    key_factor = jnp.exp(block_end[:, :, None] - cumulative).transpose(1, 2, 0)[..., None]
    weighted_k = (rotated_k.astype(jnp.float32) * key_factor).astype(jnp.bfloat16)
    updates = jnp.einsum(
        "nthd,nthe->nhde", weighted_k, value_blocks, preferred_element_type=jnp.float32
    )
    block_decay = jnp.exp(block_end).T

    def advance(carried, inputs):
        decay, update = inputs
        return (decay[:, None, None] * carried + update, carried)

    empty_state = jnp.zeros((local_heads, key_width, value_width), jnp.float32)
    local_end, local_starts = lax.scan(advance, empty_state, (block_decay, updates))
    shard_decay = jnp.exp(jnp.sum(block_end, axis=1))
    all_decay, all_state = (
        lax.all_gather(shard_decay[None].astype(jnp.bfloat16), "ep", axis=0, tiled=True).astype(
            jnp.float32
        ),
        lax.all_gather(local_end[None].astype(jnp.bfloat16), "ep", axis=0, tiled=True).astype(
            jnp.float32
        ),
    )
    ep_index = lax.axis_index("ep")

    def absorb(source, running):
        folded = all_decay[source][:, None, None] * running + all_state[source]
        return jnp.where(source < ep_index, folded, running)

    incoming = lax.fori_loop(0, all_decay.shape[0], absorb, empty_state)
    before = jnp.exp(jnp.cumsum(block_end, axis=1) - block_end).T
    starts = local_starts + before[:, :, None, None] * incoming[None]
    carried_part = jnp.einsum(
        "nthd,nhde->nthe",
        rotated_q,
        starts.astype(jnp.bfloat16),
        preferred_element_type=jnp.float32,
    )
    carried_part = carried_part * jnp.exp(cumulative).transpose(1, 2, 0)[..., None]
    scores = jnp.einsum("nthd,nshd->nhts", rotated_q, rotated_k, preferred_element_type=jnp.float32)
    block_cum = cumulative.transpose(1, 0, 2)
    spread = block_cum[:, :, :, None] - block_cum[:, :, None, :]
    lane = jnp.arange(BLOCK, dtype=jnp.int32)
    causal = lane[:, None] >= lane[None, :]
    weight = jnp.where(causal[None, None], jnp.exp(jnp.minimum(spread, 0.0)), 0.0)
    attention_weights = (scores * weight).astype(jnp.bfloat16)
    within = jnp.einsum(
        "nhts,nshe->nthe", attention_weights, value_blocks, preferred_element_type=jnp.float32
    )
    result = within + carried_part
    center = jnp.mean(result, axis=-1, keepdims=True)
    variance = jnp.mean(jnp.square(result - center), axis=-1, keepdims=True)
    normed = ((result - center) * lax.rsqrt(variance + epsilon)).astype(jnp.bfloat16)
    normed = normed.reshape(seq_rows, local_heads * value_width)
    return lax.psum_scatter(
        jnp.dot(normed, out_weight, preferred_element_type=jnp.float32).astype(jnp.bfloat16),
        "tp",
        scatter_dimension=0,
        tiled=True,
    )


def expert_part(
    expert_input, expert_gain, route_ids, route_weights, gate_weight, up_weight, down_weight
):
    tok_rows = expert_input.shape[0]
    tp_count = lax.axis_size("tp")
    count_experts = lax.axis_size("ep")
    tok_local = tok_rows // tp_count
    choose = route_ids.shape[1]
    capacity = 9 * choose * tok_local // (8 * count_experts)
    width = expert_input.shape[1]
    widened = expert_input.astype(jnp.float32)
    normed = (
        widened
        * lax.rsqrt(jnp.mean(widened * widened, axis=-1, keepdims=True) + epsilon)
        * expert_gain
    ).astype(jnp.bfloat16)
    flat_routes = route_ids.reshape(tp_count, tok_local * choose)
    onehot = (
        flat_routes[:, :, None] == jnp.arange(count_experts, dtype=jnp.int32)[None, None, :]
    ).astype(jnp.int32)
    ranks = jnp.sum(jnp.cumsum(onehot, axis=1) * onehot, axis=-1) - 1
    tp_index = lax.axis_index("tp")
    own_routes = flat_routes[tp_index]
    own_ranks = ranks[tp_index]
    pair_token = jnp.arange(tok_local * choose, dtype=jnp.int32) // choose
    gate_local = gate_weight[0]
    up_local = up_weight[0]
    down_local = down_weight[0]
    owners = jnp.arange(tp_count, dtype=jnp.int32)[:, None]
    slot_index = ((owners * count_experts + flat_routes) * capacity + ranks).reshape(-1)
    source_token = (owners * tok_local + pair_token[None, :]).reshape(-1)
    table_size = tp_count * count_experts * capacity
    slot_token = jnp.zeros((table_size,), jnp.int32).at[slot_index].set(source_token)
    filled = jnp.zeros((table_size,), jnp.bfloat16).at[slot_index].set(1.0)
    outgoing = (normed[slot_token] * filled[:, None]).reshape(
        tp_count, count_experts, capacity, width
    )
    arrived = lax.all_to_all(outgoing, "ep", split_axis=1, concat_axis=1, tiled=True).reshape(
        -1, width
    )
    gate_part = jnp.dot(arrived, gate_local, preferred_element_type=jnp.float32)
    up_part = jnp.dot(arrived, up_local, preferred_element_type=jnp.float32)
    hidden = (jax.nn.silu(gate_part) * up_part).astype(jnp.bfloat16)
    summed = lax.psum_scatter(
        jnp.dot(hidden, down_local, preferred_element_type=jnp.float32).astype(jnp.bfloat16),
        "tp",
        scatter_dimension=0,
        tiled=True,
    ).astype(jnp.float32)
    summed = summed.astype(jnp.bfloat16).reshape(count_experts, capacity, width)
    returned = lax.all_to_all(summed, "ep", split_axis=0, concat_axis=0, tiled=True).reshape(
        count_experts * capacity, width
    )
    picked = returned[own_routes * capacity + own_ranks].reshape(tok_local, choose, width)
    own_weights = route_weights.reshape(tp_count, tok_local, choose)[tp_index]
    combined = jnp.sum(picked.astype(jnp.float32) * own_weights[:, :, None], axis=1)
    return combined.astype(jnp.bfloat16)


def shards(
    queries,
    key_rows,
    values,
    log_decay,
    out_weight,
    expert_input,
    expert_gain,
    route_ids,
    route_weights,
    gate_weight,
    up_weight,
    down_weight,
):
    mixer_out = retention_part(queries, key_rows, values, log_decay, out_weight)
    expert_out = expert_part(
        expert_input, expert_gain, route_ids, route_weights, gate_weight, up_weight, down_weight
    )
    return (mixer_out, expert_out)


def swap(tensor, axis, bit):
    count = lax.axis_size(axis)
    return lax.ppermute(tensor, axis, [(i, i ^ bit) for i in range(count)])


def added(one, other):
    return (one.astype(jnp.float32) + other.astype(jnp.float32)).astype(jnp.bfloat16)


def relative_blocks(tensor, axis):
    count = lax.axis_size(axis)
    rows = tensor.shape[0] // count
    own = lax.axis_index(axis)
    return [
        lax.dynamic_slice_in_dim(tensor, (own ^ d) * rows, rows, axis=0) for d in range(count)
    ]


def halve(tensor, axis, at=0):
    bit = 1
    while tensor.shape[at] > 1:
        lead = (slice(None),) * at
        away = tensor[lead + (slice(1, None, 2),)]
        kept = tensor[lead + (slice(0, None, 2),)]
        tensor = added(kept, swap(away, axis, bit))
        bit *= 2
    return tensor


def prefix_state(decay, state):
    count = lax.axis_size("ep")
    ep_index = lax.axis_index("ep")
    total_decay, total = decay, state
    before = jnp.zeros_like(state)
    bit = 1
    while bit < count:
        upper = (ep_index & bit) > 0
        last = bit * 2 >= count
        pairs = [(i, i ^ bit) for i in range(count) if not last or not i & bit]
        other = lax.ppermute(total.astype(jnp.bfloat16), "ep", pairs).astype(jnp.float32)
        gained = jnp.where(upper, other, 0.0)
        if bit == 1:
            between = jnp.ones_like(decay)
        before = before + between[:, None, None] * gained
        if not last:
            other_decay = lax.ppermute(total_decay, "ep", pairs)
            own_factor = jnp.where(upper, 1.0, other_decay)
            other_factor = jnp.where(upper, total_decay, 1.0)
            total = own_factor[:, None, None] * total + other_factor[:, None, None] * other
            between = between * jnp.where(upper, other_decay, 1.0)
            total_decay = total_decay * other_decay
        bit *= 2
    return before


def retention_swapped(queries, key_rows, values, log_decay, out_weight):
    seq_rows = queries.shape[0]
    heads = log_decay.shape[0]
    key_width = queries.shape[1] // heads
    value_width = values.shape[1] // heads
    blocks = seq_rows // BLOCK
    position_indices = lax.axis_index("ep") * seq_rows + jnp.arange(seq_rows, dtype=jnp.int32)
    rotated_q = rotate(
        queries.astype(jnp.float32).reshape(seq_rows, heads, key_width), position_indices
    ).astype(jnp.bfloat16).reshape(seq_rows, heads * key_width)
    rotated_k = (
        rotate(key_rows.astype(jnp.float32).reshape(seq_rows, heads, key_width), position_indices)
        * key_width ** (-0.5)
    ).astype(jnp.bfloat16).reshape(seq_rows, heads * key_width)
    cumulative = jnp.cumsum(log_decay.reshape(heads, blocks, BLOCK), axis=-1)
    block_end = cumulative[:, :, -1]
    lane = jnp.arange(BLOCK, dtype=jnp.int32)
    causal = lane[:, None] >= lane[None, :]

    def tile(tensor, block, head, width):
        return tensor[block * BLOCK : (block + 1) * BLOCK, head * width : (head + 1) * width]

    starts, ends = [], []
    for head in range(heads):
        carried = jnp.zeros((key_width, value_width), jnp.float32)
        for block in range(blocks):
            starts.append(carried)
            factor = jnp.exp(block_end[head, block] - cumulative[head, block])[:, None]
            weighted = (
                tile(rotated_k, block, head, key_width).astype(jnp.float32) * factor
            ).astype(jnp.bfloat16)
            update = lax.dot_general(
                weighted,
                tile(values, block, head, value_width),
                (((0,), (0,)), ((), ())),
                preferred_element_type=jnp.float32,
            )
            carried = jnp.exp(block_end[head, block]) * carried + update
        ends.append(carried)
    shard_decay = jnp.exp(jnp.sum(block_end, axis=1))
    incoming = prefix_state(shard_decay, jnp.stack(ends))
    before = jnp.exp(jnp.cumsum(block_end, axis=1) - block_end)
    columns = []
    for head in range(heads):
        pieces = []
        for block in range(blocks):
            start = starts[head * blocks + block] + before[head, block] * incoming[head]
            query = tile(rotated_q, block, head, key_width)
            total = cumulative[head, block]
            carried_part = jnp.dot(
                query, start.astype(jnp.bfloat16), preferred_element_type=jnp.float32
            ) * jnp.exp(total)[:, None]
            scores = lax.dot_general(
                query,
                tile(rotated_k, block, head, key_width),
                (((1,), (1,)), ((), ())),
                preferred_element_type=jnp.float32,
            )
            spread = total[:, None] - total[None, :]
            weight = jnp.where(causal, jnp.exp(jnp.minimum(spread, 0.0)), 0.0)
            within = jnp.dot(
                (scores * weight).astype(jnp.bfloat16),
                tile(values, block, head, value_width),
                preferred_element_type=jnp.float32,
            )
            result = within + carried_part
            center = jnp.mean(result, axis=-1, keepdims=True)
            variance = jnp.mean(jnp.square(result - center), axis=-1, keepdims=True)
            pieces.append(((result - center) * lax.rsqrt(variance + epsilon)).astype(jnp.bfloat16))
        columns.append(jnp.concatenate(pieces, axis=0))
    normed = jnp.concatenate(columns, axis=1)
    partial = jnp.dot(normed, out_weight, preferred_element_type=jnp.float32).astype(jnp.bfloat16)
    return halve(jnp.stack(relative_blocks(partial, "tp")), "tp")[0]


PIECES = 2
COLUMN_CHUNKS = 4
FIRST_ALONG_TP = 1


def expert_dense(
    expert_input, expert_gain, route_ids, route_weights, gate_weight, up_weight, down_weight
):
    tok_rows, width = expert_input.shape
    tp_count = lax.axis_size("tp")
    count_experts = lax.axis_size("ep")
    tok_local = tok_rows // tp_count
    choose = route_ids.shape[1]
    capacity = 9 * choose * tok_local // (8 * count_experts)
    own_expert = lax.axis_index("ep").astype(jnp.float32)
    gate_local, up_local, down_local = gate_weight[0], up_weight[0], down_weight[0]

    own = relative_blocks(expert_input, "tp")
    rows = tok_local // PIECES
    straight, passed = {}, {}
    for d in range(0, tp_count, 2):
        got = [swap(own[d][i * rows : (i + 1) * rows], "ep", 2) for i in range(PIECES)]
        straight[d] = jnp.concatenate(got)
        passed[d + 1] = jnp.concatenate([swap(piece, "tp", 1) for piece in got])
    straight_two = swap(jnp.stack([straight[d] for d in sorted(straight)]), "ep", 1)
    passed_two = swap(jnp.stack([passed[d] for d in sorted(passed)]), "ep", 1)
    own_all = jnp.stack(own)
    beside = swap(own_all, "ep", 1)
    near_rows = jnp.concatenate([own_all, beside])
    far, far_two = [], []
    for d in range(tp_count):
        far.append(passed[d] if d % 2 else straight[d])
        far_two.append((passed_two if d % 2 else straight_two)[d // 2])
    far_rows = jnp.stack(far + far_two)

    table = jnp.concatenate([route_ids.astype(jnp.float32), route_weights], axis=1)
    table = jnp.stack(relative_blocks(table, "tp"))
    near_table = jnp.concatenate([table, swap(table, "ep", 1)])
    far_table = jnp.concatenate([swap(table, "ep", 2), swap(table, "ep", 3)])
    place = jnp.arange(tok_local, dtype=jnp.int32)
    upper = (place[:, None] <= place[None, :]).astype(jnp.bfloat16)
    slots = jnp.arange(capacity, dtype=jnp.float32)

    def hidden_of(tokens, known):
        named = known[..., :choose] == own_expert
        chosen = jnp.any(named, axis=-1)
        weight = jnp.sum(jnp.where(named, known[..., choose:], 0.0), axis=-1)
        rank = jnp.dot(chosen.astype(jnp.bfloat16), upper, preferred_element_type=jnp.float32) - 1.0
        pick = (rank[:, None, :] == slots[None, :, None]) & chosen[:, None, :]
        slot_weight = jnp.sum(jnp.where(pick, weight[:, None, :], 0.0), axis=-1)
        pick = pick.astype(jnp.bfloat16)
        taken = jnp.einsum("bst,btd->bsd", pick, tokens, preferred_element_type=jnp.float32)
        taken = taken.reshape(-1, width)
        normed = (
            taken
            * lax.rsqrt(jnp.mean(taken * taken, axis=-1, keepdims=True) + epsilon)
            * expert_gain
        ).astype(jnp.bfloat16)
        gate_part = jnp.dot(normed, gate_local, preferred_element_type=jnp.float32)
        up_part = jnp.dot(normed, up_local, preferred_element_type=jnp.float32)
        hidden = jax.nn.silu(gate_part) * up_part * slot_weight.reshape(-1, 1)
        return hidden.astype(jnp.bfloat16), pick

    near_hidden, near_pick = hidden_of(near_rows, near_table)
    far_hidden, far_pick = hidden_of(far_rows, far_table)

    def result_of(hidden, pick, down_part):
        partial = jnp.dot(hidden, down_part, preferred_element_type=jnp.float32)
        partial = partial.astype(jnp.bfloat16).reshape(-1, capacity, down_part.shape[1])
        spread = jnp.einsum("bst,bsd->btd", pick, partial, preferred_element_type=jnp.float32)
        return spread.astype(jnp.bfloat16).reshape(2, tp_count, tok_local, -1)

    finished = []
    chunk = width // COLUMN_CHUNKS
    for index in range(COLUMN_CHUNKS):
        down_part = down_local[:, index * chunk : (index + 1) * chunk]
        far_part = result_of(far_hidden, far_pick, down_part)
        near_part = result_of(near_hidden, near_pick, down_part)
        far_sum = added(far_part[0], swap(far_part[1], "ep", 1))
        near_sum = added(near_part[0], swap(near_part[1], "ep", 1))
        if index < FIRST_ALONG_TP:
            both = halve(jnp.stack([far_sum, near_sum]), "tp", 1)
            finished.append(added(both[1], swap(both[0], "ep", 2))[0])
        else:
            finished.append(halve(added(near_sum, swap(far_sum, "ep", 2)), "tp")[0])
    return jnp.concatenate(finished, axis=1)


def shards_dense(
    queries,
    key_rows,
    values,
    log_decay,
    out_weight,
    expert_input,
    expert_gain,
    route_ids,
    route_weights,
    gate_weight,
    up_weight,
    down_weight,
):
    mixer_out = retention_swapped(queries, key_rows, values, log_decay, out_weight)
    expert_out = expert_dense(
        expert_input, expert_gain, route_ids, route_weights, gate_weight, up_weight, down_weight
    )
    return (mixer_out, expert_out)


def fits_dense(mesh):
    ep_count, tp_count = mesh.shape["ep"], mesh.shape["tp"]
    return ep_count == 4 and tp_count >= 2 and tp_count & (tp_count - 1) == 0


def solution(mesh):
    return jax.shard_map(
        shards_dense if fits_dense(mesh) else shards,
        mesh=mesh,
        in_specs=(
            P(("grp", "ep"), "tp"),
            P(("grp", "ep"), "tp"),
            P(("grp", "ep"), "tp"),
            P("tp", "ep"),
            P("tp", None),
            P(("grp", "ep"), None),
            P(),
            P(("grp", "ep"), None),
            P(("grp", "ep"), None),
            P("ep", None, "tp"),
            P("ep", None, "tp"),
            P("ep", "tp", None),
        ),
        out_specs=(P(("grp", "ep", "tp"), None), P(("grp", "ep", "tp"), None)),
        check_vma=False,
    )
```

```python
import jax
import jax.numpy as jnp
from jax import lax
from jax.experimental import pallas as pl
from jax.experimental.pallas import tpu as pltpu
from jax.sharding import PartitionSpec as P

BLOCK = 256


epsilon = 1e-06
rope_base = 10000.0


def rotate(tensor, position_indices):
    width = tensor.shape[-1]
    middle = width // 2
    inverse = rope_base ** (-jnp.arange(0, width, 2, dtype=jnp.float32) / width)
    angles = position_indices.astype(jnp.float32)[:, None] * inverse[None, :]
    cosine = jnp.cos(angles)[:, None, :]
    sine_part = jnp.sin(angles)[:, None, :]
    first_half = tensor[..., :middle]
    second_half = tensor[..., middle:]
    return jnp.concatenate(
        [
            first_half * cosine - second_half * sine_part,
            second_half * cosine + first_half * sine_part,
        ],
        axis=-1,
    )


def retention_part(queries, key_rows, values, log_decay, out_weight):
    seq_rows = queries.shape[0]
    local_heads = log_decay.shape[0]
    key_width = queries.shape[1] // local_heads
    value_width = values.shape[1] // local_heads
    blocks = seq_rows // BLOCK
    position_indices = lax.axis_index("ep") * seq_rows + jnp.arange(seq_rows, dtype=jnp.int32)
    rotated_q = rotate(
        queries.astype(jnp.float32).reshape(seq_rows, local_heads, key_width), position_indices
    )
    rotated_q = rotated_q.astype(jnp.bfloat16).reshape(blocks, BLOCK, local_heads, key_width)
    rotated_k = rotate(
        key_rows.astype(jnp.float32).reshape(seq_rows, local_heads, key_width), position_indices
    ) * key_width ** (-0.5)
    rotated_k = rotated_k.astype(jnp.bfloat16).reshape(blocks, BLOCK, local_heads, key_width)
    value_blocks = values.reshape(blocks, BLOCK, local_heads, value_width)
    cumulative = jnp.cumsum(log_decay.reshape(local_heads, blocks, BLOCK), axis=-1)
    block_end = cumulative[:, :, -1]
    key_factor = jnp.exp(block_end[:, :, None] - cumulative).transpose(1, 2, 0)[..., None]
    weighted_k = (rotated_k.astype(jnp.float32) * key_factor).astype(jnp.bfloat16)
    updates = jnp.einsum(
        "nthd,nthe->nhde", weighted_k, value_blocks, preferred_element_type=jnp.float32
    )
    block_decay = jnp.exp(block_end).T

    def advance(carried, inputs):
        decay, update = inputs
        return (decay[:, None, None] * carried + update, carried)

    empty_state = jnp.zeros((local_heads, key_width, value_width), jnp.float32)
    local_end, local_starts = lax.scan(advance, empty_state, (block_decay, updates))
    shard_decay = jnp.exp(jnp.sum(block_end, axis=1))
    all_decay, all_state = (
        lax.all_gather(shard_decay[None].astype(jnp.bfloat16), "ep", axis=0, tiled=True).astype(
            jnp.float32
        ),
        lax.all_gather(local_end[None].astype(jnp.bfloat16), "ep", axis=0, tiled=True).astype(
            jnp.float32
        ),
    )
    ep_index = lax.axis_index("ep")

    def absorb(source, running):
        folded = all_decay[source][:, None, None] * running + all_state[source]
        return jnp.where(source < ep_index, folded, running)

    incoming = lax.fori_loop(0, all_decay.shape[0], absorb, empty_state)
    before = jnp.exp(jnp.cumsum(block_end, axis=1) - block_end).T
    starts = local_starts + before[:, :, None, None] * incoming[None]
    carried_part = jnp.einsum(
        "nthd,nhde->nthe",
        rotated_q,
        starts.astype(jnp.bfloat16),
        preferred_element_type=jnp.float32,
    )
    carried_part = carried_part * jnp.exp(cumulative).transpose(1, 2, 0)[..., None]
    scores = jnp.einsum("nthd,nshd->nhts", rotated_q, rotated_k, preferred_element_type=jnp.float32)
    block_cum = cumulative.transpose(1, 0, 2)
    spread = block_cum[:, :, :, None] - block_cum[:, :, None, :]
    lane = jnp.arange(BLOCK, dtype=jnp.int32)
    causal = lane[:, None] >= lane[None, :]
    weight = jnp.where(causal[None, None], jnp.exp(jnp.minimum(spread, 0.0)), 0.0)
    attention_weights = (scores * weight).astype(jnp.bfloat16)
    within = jnp.einsum(
        "nhts,nshe->nthe", attention_weights, value_blocks, preferred_element_type=jnp.float32
    )
    result = within + carried_part
    center = jnp.mean(result, axis=-1, keepdims=True)
    variance = jnp.mean(jnp.square(result - center), axis=-1, keepdims=True)
    normed = ((result - center) * lax.rsqrt(variance + epsilon)).astype(jnp.bfloat16)
    normed = normed.reshape(seq_rows, local_heads * value_width)
    return lax.psum_scatter(
        jnp.dot(normed, out_weight, preferred_element_type=jnp.float32).astype(jnp.bfloat16),
        "tp",
        scatter_dimension=0,
        tiled=True,
    )


def expert_part(
    expert_input, expert_gain, route_ids, route_weights, gate_weight, up_weight, down_weight
):
    tok_rows = expert_input.shape[0]
    tp_count = lax.axis_size("tp")
    count_experts = lax.axis_size("ep")
    tok_local = tok_rows // tp_count
    choose = route_ids.shape[1]
    capacity = 9 * choose * tok_local // (8 * count_experts)
    width = expert_input.shape[1]
    widened = expert_input.astype(jnp.float32)
    normed = (
        widened
        * lax.rsqrt(jnp.mean(widened * widened, axis=-1, keepdims=True) + epsilon)
        * expert_gain
    ).astype(jnp.bfloat16)
    flat_routes = route_ids.reshape(tp_count, tok_local * choose)
    onehot = (
        flat_routes[:, :, None] == jnp.arange(count_experts, dtype=jnp.int32)[None, None, :]
    ).astype(jnp.int32)
    ranks = jnp.sum(jnp.cumsum(onehot, axis=1) * onehot, axis=-1) - 1
    tp_index = lax.axis_index("tp")
    own_routes = flat_routes[tp_index]
    own_ranks = ranks[tp_index]
    pair_token = jnp.arange(tok_local * choose, dtype=jnp.int32) // choose
    gate_local = gate_weight[0]
    up_local = up_weight[0]
    down_local = down_weight[0]
    owners = jnp.arange(tp_count, dtype=jnp.int32)[:, None]
    slot_index = ((owners * count_experts + flat_routes) * capacity + ranks).reshape(-1)
    source_token = (owners * tok_local + pair_token[None, :]).reshape(-1)
    table_size = tp_count * count_experts * capacity
    slot_token = jnp.zeros((table_size,), jnp.int32).at[slot_index].set(source_token)
    filled = jnp.zeros((table_size,), jnp.bfloat16).at[slot_index].set(1.0)
    outgoing = (normed[slot_token] * filled[:, None]).reshape(
        tp_count, count_experts, capacity, width
    )
    arrived = lax.all_to_all(outgoing, "ep", split_axis=1, concat_axis=1, tiled=True).reshape(
        -1, width
    )
    gate_part = jnp.dot(arrived, gate_local, preferred_element_type=jnp.float32)
    up_part = jnp.dot(arrived, up_local, preferred_element_type=jnp.float32)
    hidden = (jax.nn.silu(gate_part) * up_part).astype(jnp.bfloat16)
    summed = lax.psum_scatter(
        jnp.dot(hidden, down_local, preferred_element_type=jnp.float32).astype(jnp.bfloat16),
        "tp",
        scatter_dimension=0,
        tiled=True,
    ).astype(jnp.float32)
    summed = summed.astype(jnp.bfloat16).reshape(count_experts, capacity, width)
    returned = lax.all_to_all(summed, "ep", split_axis=0, concat_axis=0, tiled=True).reshape(
        count_experts * capacity, width
    )
    picked = returned[own_routes * capacity + own_ranks].reshape(tok_local, choose, width)
    own_weights = route_weights.reshape(tp_count, tok_local, choose)[tp_index]
    combined = jnp.sum(picked.astype(jnp.float32) * own_weights[:, :, None], axis=1)
    return combined.astype(jnp.bfloat16)


def shards(
    queries,
    key_rows,
    values,
    log_decay,
    out_weight,
    expert_input,
    expert_gain,
    route_ids,
    route_weights,
    gate_weight,
    up_weight,
    down_weight,
):
    mixer_out = retention_part(queries, key_rows, values, log_decay, out_weight)
    expert_out = expert_part(
        expert_input, expert_gain, route_ids, route_weights, gate_weight, up_weight, down_weight
    )
    return (mixer_out, expert_out)


def swap(tensor, axis, bit):
    count = lax.axis_size(axis)
    return lax.ppermute(tensor, axis, [(i, i ^ bit) for i in range(count)])


def added(one, other):
    return (one.astype(jnp.float32) + other.astype(jnp.float32)).astype(jnp.bfloat16)


def halve(tensor, axis, at=0, after=None):
    own = lax.axis_index(axis)
    bit = 0
    while tensor.shape[at] > 1:
        shape = tensor.shape
        tensor = tensor.reshape(shape[:at] + (shape[at] // 2, 2) + shape[at + 1 :])
        side = (own >> bit) & 1
        away = lax.dynamic_index_in_dim(tensor, 1 - side, at + 1, keepdims=False)
        kept = lax.dynamic_index_in_dim(tensor, side, at + 1, keepdims=False)
        came = swap(away, axis, 1 << bit)
        if after is not None and bit < len(after):
            came, _ = lax.optimization_barrier((came, after[bit]))
        tensor = added(kept, came)
        bit += 1
    return tensor


def prefix_state(decay, state, sent):
    count = lax.axis_size("ep")
    ep_index = lax.axis_index("ep")
    total_decay, total = decay, state
    before = jnp.zeros_like(state)
    bit = 1
    while bit < count:
        upper = (ep_index & bit) > 0
        last = bit * 2 >= count
        pairs = [(i, i ^ bit) for i in range(count) if not last or not i & bit]
        other = lax.ppermute(sent, "ep", pairs).astype(jnp.float32)
        gained = jnp.where(upper, other, 0.0)
        if bit == 1:
            between = jnp.ones_like(decay)
        before = before + between[:, None, None] * gained
        if not last:
            other_decay = lax.ppermute(total_decay, "ep", pairs)
            own_factor = jnp.where(upper, 1.0, other_decay)
            other_factor = jnp.where(upper, total_decay, 1.0)
            total = own_factor[:, None, None] * total + other_factor[:, None, None] * other
            between = between * jnp.where(upper, other_decay, 1.0)
            total_decay = total_decay * other_decay
            sent = total.astype(jnp.bfloat16)
        bit *= 2
    return before


def inner_kernel(q_ref, k_ref, v_ref, cos_ref, sin_ref, col_ref, row_ref, turned_ref, within_ref, state_ref, sent_ref):
    cosine, sine_part = cos_ref[...], sin_ref[...]
    middle = cosine.shape[1]

    def turn(ref, scale):
        first = ref[:, :middle].astype(jnp.float32)
        second = ref[:, middle:].astype(jnp.float32)
        both = jnp.concatenate(
            [first * cosine - second * sine_part, second * cosine + first * sine_part], axis=1
        )
        return both * scale

    query = turn(q_ref, 1.0).astype(jnp.bfloat16)
    key = turn(k_ref, (2 * middle) ** (-0.5)).astype(jnp.bfloat16)
    value = v_ref[...]
    column, row = col_ref[0], row_ref[0]
    turned_ref[...] = query
    end = row[:, -1:]
    weighted = (key.astype(jnp.float32) * jnp.exp(end - column)).astype(jnp.bfloat16)
    state = lax.dot_general(
        weighted, value, (((0,), (0,)), ((), ())), preferred_element_type=jnp.float32
    )
    state_ref[0] = state
    sent_ref[0] = state.astype(jnp.bfloat16)
    scores = lax.dot_general(
        query, key, (((1,), (1,)), ((), ())), preferred_element_type=jnp.float32
    )
    rows = lax.broadcasted_iota(jnp.int32, scores.shape, 0)
    lanes = lax.broadcasted_iota(jnp.int32, scores.shape, 1)
    weight = jnp.where(rows >= lanes, jnp.exp(jnp.minimum(column - row, 0.0)), 0.0)
    within_ref[...] = jnp.dot(
        (scores * weight).astype(jnp.bfloat16), value, preferred_element_type=jnp.float32
    )


def outer_kernel(turned_ref, start_ref, col_ref, within_ref, normed_ref):
    carried_part = jnp.dot(
        turned_ref[...], start_ref[0].astype(jnp.bfloat16), preferred_element_type=jnp.float32
    )
    result = within_ref[...] + carried_part * jnp.exp(col_ref[0])
    center = jnp.mean(result, axis=-1, keepdims=True)
    result = result - center
    variance = jnp.mean(result * result, axis=-1, keepdims=True)
    normed_ref[...] = (result * lax.rsqrt(variance + epsilon)).astype(jnp.bfloat16)


def retention_inner(queries, key_rows, values, log_decay):
    seq_rows = queries.shape[0]
    heads = log_decay.shape[0]
    kw, vw = queries.shape[1] // heads, values.shape[1] // heads
    position_indices = lax.axis_index("ep") * seq_rows + jnp.arange(seq_rows, dtype=jnp.int32)
    inverse = rope_base ** (-jnp.arange(0, kw, 2, dtype=jnp.float32) / kw)
    angles = position_indices.astype(jnp.float32)[:, None] * inverse[None, :]
    cumulative = jnp.cumsum(log_decay, axis=-1)
    column, row = cumulative[:, :, None], cumulative[:, None, :]
    side = lambda width: pl.BlockSpec((seq_rows, width), lambda h: (0, h))
    table = pl.BlockSpec((seq_rows, kw // 2), lambda h: (0, 0))
    head_state = pl.BlockSpec((1, kw, vw), lambda h: (h, 0, 0))
    turned, within, state, sent = pl.pallas_call(
        inner_kernel,
        grid=(heads,),
        in_specs=[
            side(kw), side(kw), side(vw), table, table,
            pl.BlockSpec((1, seq_rows, 1), lambda h: (h, 0, 0)),
            pl.BlockSpec((1, 1, seq_rows), lambda h: (h, 0, 0)),
        ],
        out_specs=[side(kw), side(vw), head_state, head_state],
        out_shape=[
            jax.ShapeDtypeStruct((seq_rows, heads * kw), jnp.bfloat16),
            jax.ShapeDtypeStruct((seq_rows, heads * vw), jnp.float32),
            jax.ShapeDtypeStruct((heads, kw, vw), jnp.float32),
            jax.ShapeDtypeStruct((heads, kw, vw), jnp.bfloat16),
        ],
        cost_estimate=pl.CostEstimate(flops=4 * 10**9, bytes_accessed=10**7, transcendentals=0),
    )(queries, key_rows, values, jnp.cos(angles), jnp.sin(angles), column, row)
    decay = jnp.exp(cumulative[:, -1])
    return turned, within, column, decay, state, sent


def retention_outer(turned, within, column, incoming, out_weight):
    seq_rows = turned.shape[0]
    heads, kw, vw = incoming.shape
    side = lambda width: pl.BlockSpec((seq_rows, width), lambda h: (0, h))
    normed = pl.pallas_call(
        outer_kernel,
        grid=(heads,),
        in_specs=[
            side(kw),
            pl.BlockSpec((1, kw, vw), lambda h: (h, 0, 0)),
            pl.BlockSpec((1, seq_rows, 1), lambda h: (h, 0, 0)),
            side(vw),
        ],
        out_specs=side(vw),
        out_shape=jax.ShapeDtypeStruct((seq_rows, heads * vw), jnp.bfloat16),
        cost_estimate=pl.CostEstimate(flops=2 * 10**9, bytes_accessed=10**7, transcendentals=0),
    )(turned, incoming, column, within)
    return jnp.dot(normed, out_weight, preferred_element_type=jnp.float32).astype(jnp.bfloat16)


PIECES = 2
COLUMN_CHUNKS = 4
FIRST_ALONG_TP = 2


def expert_dense(
    inner,
    out_weight,
    expert_input,
    expert_gain,
    route_ids,
    route_weights,
    gate_weight,
    up_weight,
    down_weight,
):
    tok_rows, width = expert_input.shape
    tp_count = lax.axis_size("tp")
    count_experts = lax.axis_size("ep")
    tok_local = tok_rows // tp_count
    choose = route_ids.shape[1]
    capacity = 9 * choose * tok_local // (8 * count_experts)
    own_expert = lax.axis_index("ep").astype(jnp.float32)
    gate_local, up_local, down_local = gate_weight[0], up_weight[0], down_weight[0]

    side = lax.axis_index("tp") & 1
    half = width // 2
    sent = lax.dynamic_slice_in_dim(expert_input, side * half, half, axis=1)
    rows = tok_rows // PIECES
    straight = [swap(sent[i * rows : (i + 1) * rows], "ep", 2) for i in range(PIECES)]
    beside = swap(expert_input, "ep", 1)
    passed = [swap(piece, "tp", 1) for piece in straight]
    straight = straight + [swap(piece, "ep", 1) for piece in straight]
    passed = passed + [swap(piece, "ep", 1) for piece in passed]

    table = jnp.concatenate([route_ids.astype(jnp.float32), route_weights], axis=1)
    table = table.reshape(tp_count, tok_local, 2 * choose)
    near_table = jnp.concatenate([table, swap(table, "ep", 1)])
    far_table = jnp.concatenate([swap(table, "ep", 2), swap(table, "ep", 3)])
    place = jnp.arange(tok_local, dtype=jnp.int32)
    upper = (place[:, None] <= place[None, :]).astype(jnp.bfloat16)
    slots = jnp.arange(capacity, dtype=jnp.float32)

    def picks(known):
        named = known[..., :choose] == own_expert
        chosen = jnp.any(named, axis=-1)
        weight = jnp.sum(jnp.where(named, known[..., choose:], 0.0), axis=-1)
        rank = jnp.dot(chosen.astype(jnp.bfloat16), upper, preferred_element_type=jnp.float32) - 1.0
        pick = (rank[:, None, :] == slots[None, :, None]) & chosen[:, None, :]
        slot_weight = jnp.sum(jnp.where(pick, weight[:, None, :], 0.0), axis=-1)
        return pick.astype(jnp.bfloat16), slot_weight.reshape(-1, 1)

    def select(pick, pieces):
        count = pick.shape[0] // len(pieces)
        return jnp.concatenate(
            [
                jnp.einsum(
                    "bst,btd->bsd",
                    pick[i * count : (i + 1) * count],
                    piece.reshape(count, tok_local, -1),
                    preferred_element_type=jnp.float32,
                ).astype(jnp.bfloat16)
                for i, piece in enumerate(pieces)
            ]
        ).reshape(2 * tp_count * capacity, -1)

    def hidden_of(taken, slot_weight):
        taken = taken.astype(jnp.float32)
        normed = (
            taken
            * lax.rsqrt(jnp.mean(taken * taken, axis=-1, keepdims=True) + epsilon)
            * expert_gain
        ).astype(jnp.bfloat16)
        gate_part = jnp.dot(normed, gate_local, preferred_element_type=jnp.float32)
        up_part = jnp.dot(normed, up_local, preferred_element_type=jnp.float32)
        return (jax.nn.silu(gate_part) * up_part * slot_weight).astype(jnp.bfloat16)

    near_pick, near_weight = picks(near_table)
    far_pick, far_weight = picks(far_table)
    near_hidden = hidden_of(select(near_pick, [expert_input, beside]), near_weight)
    turned, within, column, incoming = inner
    incoming, near_hidden = lax.optimization_barrier((incoming, near_hidden))
    mixer_part = retention_outer(turned, within, column, incoming, out_weight)
    one, other = select(far_pick, straight), select(far_pick, passed)
    taken = jnp.concatenate(
        [jnp.where(side == 0, one, other), jnp.where(side == 0, other, one)], axis=1
    )
    taken, near_hidden, mixer_part = lax.optimization_barrier((taken, near_hidden, mixer_part))
    far_hidden = hidden_of(taken, far_weight)
    mixer_part = mixer_part.reshape(tp_count, -1, mixer_part.shape[1])
    mixer_out = halve(mixer_part, "tp", after=[far_hidden])[0]

    def result_of(hidden, pick, down_part):
        partial = jnp.dot(hidden, down_part, preferred_element_type=jnp.float32)
        partial = partial.astype(jnp.bfloat16).reshape(-1, capacity, down_part.shape[1])
        spread = jnp.einsum("bst,bsd->btd", pick, partial, preferred_element_type=jnp.float32)
        return spread.astype(jnp.bfloat16).reshape(2, tp_count, tok_local, -1)

    finished = []
    chunk = width // COLUMN_CHUNKS
    for index in range(COLUMN_CHUNKS):
        down_part = down_local[:, index * chunk : (index + 1) * chunk]
        far_part = result_of(far_hidden, far_pick, down_part)
        near_part = result_of(near_hidden, near_pick, down_part)
        far_sum = added(far_part[0], swap(far_part[1], "ep", 1))
        near_sum = added(near_part[0], swap(near_part[1], "ep", 1))
        if index < FIRST_ALONG_TP:
            both = halve(jnp.stack([far_sum, near_sum]), "tp", 1)
            finished.append(added(both[1], swap(both[0], "ep", 2))[0])
        else:
            finished.append(halve(added(near_sum, swap(far_sum, "ep", 2)), "tp")[0])
    return mixer_out, jnp.concatenate(finished, axis=1)


def shards_dense(
    queries,
    key_rows,
    values,
    log_decay,
    out_weight,
    expert_input,
    expert_gain,
    route_ids,
    route_weights,
    gate_weight,
    up_weight,
    down_weight,
):
    turned, within, column, decay, state, sent = retention_inner(
        queries, key_rows, values, log_decay
    )
    inner = (turned, within, column, prefix_state(decay, state, sent))
    return expert_dense(
        inner,
        out_weight,
        expert_input,
        expert_gain,
        route_ids,
        route_weights,
        gate_weight,
        up_weight,
        down_weight,
    )


def fits_dense(mesh):
    ep_count, tp_count = mesh.shape["ep"], mesh.shape["tp"]
    return ep_count == 4 and tp_count >= 2 and tp_count & (tp_count - 1) == 0


def solution(mesh):
    return jax.shard_map(
        shards_dense if fits_dense(mesh) else shards,
        mesh=mesh,
        in_specs=(
            P(("grp", "ep"), "tp"),
            P(("grp", "ep"), "tp"),
            P(("grp", "ep"), "tp"),
            P("tp", "ep"),
            P("tp", None),
            P(("grp", "ep"), None),
            P(),
            P(("grp", "ep"), None),
            P(("grp", "ep"), None),
            P("ep", None, "tp"),
            P("ep", None, "tp"),
            P("ep", "tp", None),
        ),
        out_specs=(P(("grp", "ep", "tp"), None), P(("grp", "ep", "tp"), None)),
        check_vma=False,
    )
```

```python
import jax
import jax.numpy as jnp
from jax import lax
from jax.experimental import pallas as pl
from jax.sharding import PartitionSpec as P

BLOCK = 256


epsilon = 1e-06
rope_base = 10000.0


def rotate(tensor, position_indices):
    width = tensor.shape[-1]
    middle = width // 2
    inverse = rope_base ** (-jnp.arange(0, width, 2, dtype=jnp.float32) / width)
    angles = position_indices.astype(jnp.float32)[:, None] * inverse[None, :]
    cosine = jnp.cos(angles)[:, None, :]
    sine_part = jnp.sin(angles)[:, None, :]
    first_half = tensor[..., :middle]
    second_half = tensor[..., middle:]
    return jnp.concatenate(
        [
            first_half * cosine - second_half * sine_part,
            second_half * cosine + first_half * sine_part,
        ],
        axis=-1,
    )


def retention_part(queries, key_rows, values, log_decay, out_weight):
    seq_rows = queries.shape[0]
    local_heads = log_decay.shape[0]
    key_width = queries.shape[1] // local_heads
    value_width = values.shape[1] // local_heads
    blocks = seq_rows // BLOCK
    position_indices = lax.axis_index("ep") * seq_rows + jnp.arange(seq_rows, dtype=jnp.int32)
    rotated_q = rotate(
        queries.astype(jnp.float32).reshape(seq_rows, local_heads, key_width), position_indices
    )
    rotated_q = rotated_q.astype(jnp.bfloat16).reshape(blocks, BLOCK, local_heads, key_width)
    rotated_k = rotate(
        key_rows.astype(jnp.float32).reshape(seq_rows, local_heads, key_width), position_indices
    ) * key_width ** (-0.5)
    rotated_k = rotated_k.astype(jnp.bfloat16).reshape(blocks, BLOCK, local_heads, key_width)
    value_blocks = values.reshape(blocks, BLOCK, local_heads, value_width)
    cumulative = jnp.cumsum(log_decay.reshape(local_heads, blocks, BLOCK), axis=-1)
    block_end = cumulative[:, :, -1]
    key_factor = jnp.exp(block_end[:, :, None] - cumulative).transpose(1, 2, 0)[..., None]
    weighted_k = (rotated_k.astype(jnp.float32) * key_factor).astype(jnp.bfloat16)
    updates = jnp.einsum(
        "nthd,nthe->nhde", weighted_k, value_blocks, preferred_element_type=jnp.float32
    )
    block_decay = jnp.exp(block_end).T

    def advance(carried, inputs):
        decay, update = inputs
        return (decay[:, None, None] * carried + update, carried)

    empty_state = jnp.zeros((local_heads, key_width, value_width), jnp.float32)
    local_end, local_starts = lax.scan(advance, empty_state, (block_decay, updates))
    shard_decay = jnp.exp(jnp.sum(block_end, axis=1))
    all_decay, all_state = (
        lax.all_gather(shard_decay[None].astype(jnp.bfloat16), "ep", axis=0, tiled=True).astype(
            jnp.float32
        ),
        lax.all_gather(local_end[None].astype(jnp.bfloat16), "ep", axis=0, tiled=True).astype(
            jnp.float32
        ),
    )
    ep_index = lax.axis_index("ep")

    def absorb(source, running):
        folded = all_decay[source][:, None, None] * running + all_state[source]
        return jnp.where(source < ep_index, folded, running)

    incoming = lax.fori_loop(0, all_decay.shape[0], absorb, empty_state)
    before = jnp.exp(jnp.cumsum(block_end, axis=1) - block_end).T
    starts = local_starts + before[:, :, None, None] * incoming[None]
    carried_part = jnp.einsum(
        "nthd,nhde->nthe",
        rotated_q,
        starts.astype(jnp.bfloat16),
        preferred_element_type=jnp.float32,
    )
    carried_part = carried_part * jnp.exp(cumulative).transpose(1, 2, 0)[..., None]
    scores = jnp.einsum("nthd,nshd->nhts", rotated_q, rotated_k, preferred_element_type=jnp.float32)
    block_cum = cumulative.transpose(1, 0, 2)
    spread = block_cum[:, :, :, None] - block_cum[:, :, None, :]
    lane = jnp.arange(BLOCK, dtype=jnp.int32)
    causal = lane[:, None] >= lane[None, :]
    weight = jnp.where(causal[None, None], jnp.exp(jnp.minimum(spread, 0.0)), 0.0)
    attention_weights = (scores * weight).astype(jnp.bfloat16)
    within = jnp.einsum(
        "nhts,nshe->nthe", attention_weights, value_blocks, preferred_element_type=jnp.float32
    )
    result = within + carried_part
    center = jnp.mean(result, axis=-1, keepdims=True)
    variance = jnp.mean(jnp.square(result - center), axis=-1, keepdims=True)
    normed = ((result - center) * lax.rsqrt(variance + epsilon)).astype(jnp.bfloat16)
    normed = normed.reshape(seq_rows, local_heads * value_width)
    return lax.psum_scatter(
        jnp.dot(normed, out_weight, preferred_element_type=jnp.float32).astype(jnp.bfloat16),
        "tp",
        scatter_dimension=0,
        tiled=True,
    )


def expert_part(
    expert_input, expert_gain, route_ids, route_weights, gate_weight, up_weight, down_weight
):
    tok_rows = expert_input.shape[0]
    tp_count = lax.axis_size("tp")
    count_experts = lax.axis_size("ep")
    tok_local = tok_rows // tp_count
    choose = route_ids.shape[1]
    capacity = 9 * choose * tok_local // (8 * count_experts)
    width = expert_input.shape[1]
    widened = expert_input.astype(jnp.float32)
    normed = (
        widened
        * lax.rsqrt(jnp.mean(widened * widened, axis=-1, keepdims=True) + epsilon)
        * expert_gain
    ).astype(jnp.bfloat16)
    flat_routes = route_ids.reshape(tp_count, tok_local * choose)
    onehot = (
        flat_routes[:, :, None] == jnp.arange(count_experts, dtype=jnp.int32)[None, None, :]
    ).astype(jnp.int32)
    ranks = jnp.sum(jnp.cumsum(onehot, axis=1) * onehot, axis=-1) - 1
    tp_index = lax.axis_index("tp")
    own_routes = flat_routes[tp_index]
    own_ranks = ranks[tp_index]
    pair_token = jnp.arange(tok_local * choose, dtype=jnp.int32) // choose
    gate_local = gate_weight[0]
    up_local = up_weight[0]
    down_local = down_weight[0]
    owners = jnp.arange(tp_count, dtype=jnp.int32)[:, None]
    slot_index = ((owners * count_experts + flat_routes) * capacity + ranks).reshape(-1)
    source_token = (owners * tok_local + pair_token[None, :]).reshape(-1)
    table_size = tp_count * count_experts * capacity
    slot_token = jnp.zeros((table_size,), jnp.int32).at[slot_index].set(source_token)
    filled = jnp.zeros((table_size,), jnp.bfloat16).at[slot_index].set(1.0)
    outgoing = (normed[slot_token] * filled[:, None]).reshape(
        tp_count, count_experts, capacity, width
    )
    arrived = lax.all_to_all(outgoing, "ep", split_axis=1, concat_axis=1, tiled=True).reshape(
        -1, width
    )
    gate_part = jnp.dot(arrived, gate_local, preferred_element_type=jnp.float32)
    up_part = jnp.dot(arrived, up_local, preferred_element_type=jnp.float32)
    hidden = (jax.nn.silu(gate_part) * up_part).astype(jnp.bfloat16)
    summed = lax.psum_scatter(
        jnp.dot(hidden, down_local, preferred_element_type=jnp.float32).astype(jnp.bfloat16),
        "tp",
        scatter_dimension=0,
        tiled=True,
    ).astype(jnp.float32)
    summed = summed.astype(jnp.bfloat16).reshape(count_experts, capacity, width)
    returned = lax.all_to_all(summed, "ep", split_axis=0, concat_axis=0, tiled=True).reshape(
        count_experts * capacity, width
    )
    picked = returned[own_routes * capacity + own_ranks].reshape(tok_local, choose, width)
    own_weights = route_weights.reshape(tp_count, tok_local, choose)[tp_index]
    combined = jnp.sum(picked.astype(jnp.float32) * own_weights[:, :, None], axis=1)
    return combined.astype(jnp.bfloat16)


def shards(
    queries,
    key_rows,
    values,
    log_decay,
    out_weight,
    expert_input,
    expert_gain,
    route_ids,
    route_weights,
    gate_weight,
    up_weight,
    down_weight,
):
    mixer_out = retention_part(queries, key_rows, values, log_decay, out_weight)
    expert_out = expert_part(
        expert_input, expert_gain, route_ids, route_weights, gate_weight, up_weight, down_weight
    )
    return (mixer_out, expert_out)


def swap(tensor, axis, bit):
    count = lax.axis_size(axis)
    return lax.ppermute(tensor, axis, [(i, i ^ bit) for i in range(count)])


def added(one, other):
    return (one.astype(jnp.float32) + other.astype(jnp.float32)).astype(jnp.bfloat16)


def halve(tensor, axis, at=0, after=None):
    own = lax.axis_index(axis)
    bit = 0
    while tensor.shape[at] > 1:
        shape = tensor.shape
        tensor = tensor.reshape(shape[:at] + (shape[at] // 2, 2) + shape[at + 1 :])
        side = (own >> bit) & 1
        away = lax.dynamic_index_in_dim(tensor, 1 - side, at + 1, keepdims=False)
        kept = lax.dynamic_index_in_dim(tensor, side, at + 1, keepdims=False)
        came = swap(away, axis, 1 << bit)
        if after is not None and bit < len(after):
            came, _ = lax.optimization_barrier((came, after[bit]))
        tensor = added(kept, came)
        bit += 1
    return tensor


def prefix_state(decay, state, sent):
    count = lax.axis_size("ep")
    ep_index = lax.axis_index("ep")
    total_decay, total = decay, state
    before = jnp.zeros_like(state)
    bit = 1
    while bit < count:
        upper = (ep_index & bit) > 0
        last = bit * 2 >= count
        pairs = [(i, i ^ bit) for i in range(count) if not last or not i & bit]
        other = lax.ppermute(sent, "ep", pairs).astype(jnp.float32)
        gained = jnp.where(upper, other, 0.0)
        if bit == 1:
            between = jnp.ones_like(decay)
        before = before + between[:, None, None] * gained
        if not last:
            other_decay = lax.ppermute(total_decay, "ep", pairs)
            own_factor = jnp.where(upper, 1.0, other_decay)
            other_factor = jnp.where(upper, total_decay, 1.0)
            total = own_factor[:, None, None] * total + other_factor[:, None, None] * other
            between = between * jnp.where(upper, other_decay, 1.0)
            total_decay = total_decay * other_decay
            sent = total.astype(jnp.bfloat16)
        bit *= 2
    return before


def inner_kernel(q_ref, k_ref, v_ref, cos_ref, sin_ref, col_ref, row_ref, turned_ref, within_ref, state_ref, sent_ref):
    cosine, sine_part = cos_ref[...], sin_ref[...]
    middle = cosine.shape[1]

    def turn(ref, scale):
        first = ref[:, :middle].astype(jnp.float32)
        second = ref[:, middle:].astype(jnp.float32)
        both = jnp.concatenate(
            [first * cosine - second * sine_part, second * cosine + first * sine_part], axis=1
        )
        return both * scale

    query = turn(q_ref, 1.0).astype(jnp.bfloat16)
    key = turn(k_ref, (2 * middle) ** (-0.5)).astype(jnp.bfloat16)
    value = v_ref[...]
    column, row = col_ref[0], row_ref[0]
    turned_ref[...] = query
    end = row[:, -1:]
    weighted = (key.astype(jnp.float32) * jnp.exp(end - column)).astype(jnp.bfloat16)
    state = lax.dot_general(
        weighted, value, (((0,), (0,)), ((), ())), preferred_element_type=jnp.float32
    )
    state_ref[0] = state
    sent_ref[0] = state.astype(jnp.bfloat16)
    scores = lax.dot_general(
        query, key, (((1,), (1,)), ((), ())), preferred_element_type=jnp.float32
    )
    rows = lax.broadcasted_iota(jnp.int32, scores.shape, 0)
    lanes = lax.broadcasted_iota(jnp.int32, scores.shape, 1)
    weight = jnp.where(rows >= lanes, jnp.exp(jnp.minimum(column - row, 0.0)), 0.0)
    within_ref[...] = jnp.dot(
        (scores * weight).astype(jnp.bfloat16), value, preferred_element_type=jnp.float32
    )


def outer_kernel(turned_ref, start_ref, col_ref, within_ref, normed_ref):
    carried_part = jnp.dot(
        turned_ref[...], start_ref[0].astype(jnp.bfloat16), preferred_element_type=jnp.float32
    )
    result = within_ref[...] + carried_part * jnp.exp(col_ref[0])
    center = jnp.mean(result, axis=-1, keepdims=True)
    result = result - center
    variance = jnp.mean(result * result, axis=-1, keepdims=True)
    normed_ref[...] = (result * lax.rsqrt(variance + epsilon)).astype(jnp.bfloat16)


def retention_inner(queries, key_rows, values, log_decay):
    seq_rows = queries.shape[0]
    heads = log_decay.shape[0]
    kw, vw = queries.shape[1] // heads, values.shape[1] // heads
    position_indices = lax.axis_index("ep") * seq_rows + jnp.arange(seq_rows, dtype=jnp.int32)
    inverse = rope_base ** (-jnp.arange(0, kw, 2, dtype=jnp.float32) / kw)
    angles = position_indices.astype(jnp.float32)[:, None] * inverse[None, :]
    cumulative = jnp.cumsum(log_decay, axis=-1)
    column, row = cumulative[:, :, None], cumulative[:, None, :]
    side = lambda width: pl.BlockSpec((seq_rows, width), lambda h: (0, h))
    table = pl.BlockSpec((seq_rows, kw // 2), lambda h: (0, 0))
    head_state = pl.BlockSpec((1, kw, vw), lambda h: (h, 0, 0))
    turned, within, state, sent = pl.pallas_call(
        inner_kernel,
        grid=(heads,),
        in_specs=[
            side(kw), side(kw), side(vw), table, table,
            pl.BlockSpec((1, seq_rows, 1), lambda h: (h, 0, 0)),
            pl.BlockSpec((1, 1, seq_rows), lambda h: (h, 0, 0)),
        ],
        out_specs=[side(kw), side(vw), head_state, head_state],
        out_shape=[
            jax.ShapeDtypeStruct((seq_rows, heads * kw), jnp.bfloat16),
            jax.ShapeDtypeStruct((seq_rows, heads * vw), jnp.float32),
            jax.ShapeDtypeStruct((heads, kw, vw), jnp.float32),
            jax.ShapeDtypeStruct((heads, kw, vw), jnp.bfloat16),
        ],
        cost_estimate=pl.CostEstimate(flops=4 * 10**9, bytes_accessed=10**7, transcendentals=0),
    )(queries, key_rows, values, jnp.cos(angles), jnp.sin(angles), column, row)
    decay = jnp.exp(cumulative[:, -1])
    return turned, within, column, decay, state, sent


def retention_outer(turned, within, column, incoming, out_weight):
    seq_rows = turned.shape[0]
    heads, kw, vw = incoming.shape
    side = lambda width: pl.BlockSpec((seq_rows, width), lambda h: (0, h))
    normed = pl.pallas_call(
        outer_kernel,
        grid=(heads,),
        in_specs=[
            side(kw),
            pl.BlockSpec((1, kw, vw), lambda h: (h, 0, 0)),
            pl.BlockSpec((1, seq_rows, 1), lambda h: (h, 0, 0)),
            side(vw),
        ],
        out_specs=side(vw),
        out_shape=jax.ShapeDtypeStruct((seq_rows, heads * vw), jnp.bfloat16),
        cost_estimate=pl.CostEstimate(flops=2 * 10**9, bytes_accessed=10**7, transcendentals=0),
    )(turned, incoming, column, within)
    return jnp.dot(normed, out_weight, preferred_element_type=jnp.float32).astype(jnp.bfloat16)


PIECES = 2
COLUMN_CHUNKS = 4
FIRST_ALONG_TP = 1


def expert_dense(
    queries,
    key_rows,
    values,
    log_decay,
    out_weight,
    expert_input,
    expert_gain,
    route_ids,
    route_weights,
    gate_weight,
    up_weight,
    down_weight,
):
    tok_rows, width = expert_input.shape
    tp_count = lax.axis_size("tp")
    count_experts = lax.axis_size("ep")
    tok_local = tok_rows // tp_count
    choose = route_ids.shape[1]
    capacity = 9 * choose * tok_local // (8 * count_experts)
    own_expert = lax.axis_index("ep").astype(jnp.float32)
    gate_local, up_local, down_local = gate_weight[0], up_weight[0], down_weight[0]

    side = lax.axis_index("tp") & 1
    half = width // 2
    sent = lax.dynamic_slice_in_dim(expert_input, side * half, half, axis=1)
    queries, sent = lax.optimization_barrier((queries, sent))
    rows = tok_rows // PIECES
    beside = swap(expert_input, "ep", 1)
    turned, within, column, decay, state, state_sent = retention_inner(
        queries, key_rows, values, log_decay
    )
    pieces = [sent[i * rows : (i + 1) * rows] for i in range(PIECES)]
    pieces[-1], state_sent = lax.optimization_barrier((pieces[-1], state_sent))
    straight = []
    for piece in pieces:
        straight.append(swap(piece, "ep", 2))
    incoming = prefix_state(decay, state, state_sent)

    table = jnp.concatenate([route_ids.astype(jnp.float32), route_weights], axis=1)
    table = table.reshape(tp_count, tok_local, 2 * choose)
    near_table = jnp.concatenate([table, swap(table, "ep", 1)])
    far_table = jnp.concatenate([swap(table, "ep", 2), swap(table, "ep", 3)])
    place = jnp.arange(tok_local, dtype=jnp.int32)
    upper = (place[:, None] <= place[None, :]).astype(jnp.bfloat16)
    slots = jnp.arange(capacity, dtype=jnp.float32)

    def picks(known):
        named = known[..., :choose] == own_expert
        chosen = jnp.any(named, axis=-1)
        weight = jnp.sum(jnp.where(named, known[..., choose:], 0.0), axis=-1)
        rank = jnp.dot(chosen.astype(jnp.bfloat16), upper, preferred_element_type=jnp.float32) - 1.0
        pick = (rank[:, None, :] == slots[None, :, None]) & chosen[:, None, :]
        slot_weight = jnp.sum(jnp.where(pick, weight[:, None, :], 0.0), axis=-1)
        return pick.astype(jnp.bfloat16), slot_weight.reshape(-1, 1)

    def select(pick, pieces):
        count = pick.shape[0] // len(pieces)
        return jnp.concatenate(
            [
                jnp.einsum(
                    "bst,btd->bsd",
                    pick[i * count : (i + 1) * count],
                    piece.reshape(count, tok_local, -1),
                    preferred_element_type=jnp.float32,
                ).astype(jnp.bfloat16)
                for i, piece in enumerate(pieces)
            ]
        ).reshape(2 * tp_count * capacity, -1)

    def hidden_of(taken, slot_weight):
        taken = taken.astype(jnp.float32)
        normed = (
            taken
            * lax.rsqrt(jnp.mean(taken * taken, axis=-1, keepdims=True) + epsilon)
            * expert_gain
        ).astype(jnp.bfloat16)
        gate_part = jnp.dot(normed, gate_local, preferred_element_type=jnp.float32)
        up_part = jnp.dot(normed, up_local, preferred_element_type=jnp.float32)
        return (jax.nn.silu(gate_part) * up_part * slot_weight).astype(jnp.bfloat16)

    near_pick, near_weight = picks(near_table)
    far_pick, far_weight = picks(far_table)
    near_hidden = hidden_of(select(near_pick, [expert_input, beside]), near_weight)
    straight[-1], near_hidden = lax.optimization_barrier((straight[-1], near_hidden))
    passed = [swap(piece, "tp", 1) for piece in straight]
    mixer_part = retention_outer(turned, within, column, incoming, out_weight)
    passed[-1], mixer_part = lax.optimization_barrier((passed[-1], mixer_part))
    straight = straight + [swap(piece, "ep", 1) for piece in straight]
    passed = passed + [swap(piece, "ep", 1) for piece in passed]
    one, other = select(far_pick, straight), select(far_pick, passed)
    taken = jnp.concatenate(
        [jnp.where(side == 0, one, other), jnp.where(side == 0, other, one)], axis=1
    )
    far_hidden = hidden_of(taken, far_weight)
    mixer_part = mixer_part.reshape(tp_count, -1, mixer_part.shape[1])
    mixer_out = halve(mixer_part, "tp", after=[far_hidden])[0]

    def result_of(hidden, pick, down_part):
        partial = jnp.dot(hidden, down_part, preferred_element_type=jnp.float32)
        partial = partial.astype(jnp.bfloat16).reshape(-1, capacity, down_part.shape[1])
        spread = jnp.einsum("bst,bsd->btd", pick, partial, preferred_element_type=jnp.float32)
        return spread.astype(jnp.bfloat16).reshape(2, tp_count, tok_local, -1)

    finished = []
    chunk = width // COLUMN_CHUNKS
    for index in range(COLUMN_CHUNKS):
        down_part = down_local[:, index * chunk : (index + 1) * chunk]
        far_part = result_of(far_hidden, far_pick, down_part)
        near_part = result_of(near_hidden, near_pick, down_part)
        far_sum = added(far_part[0], swap(far_part[1], "ep", 1))
        near_sum = added(near_part[0], swap(near_part[1], "ep", 1))
        if index < FIRST_ALONG_TP:
            both = halve(jnp.stack([far_sum, near_sum]), "tp", 1)
            finished.append(added(both[1], swap(both[0], "ep", 2))[0])
        else:
            finished.append(halve(added(near_sum, swap(far_sum, "ep", 2)), "tp")[0])
    return mixer_out, jnp.concatenate(finished, axis=1)


def shards_dense(
    queries,
    key_rows,
    values,
    log_decay,
    out_weight,
    expert_input,
    expert_gain,
    route_ids,
    route_weights,
    gate_weight,
    up_weight,
    down_weight,
):
    return expert_dense(
        queries,
        key_rows,
        values,
        log_decay,
        out_weight,
        expert_input,
        expert_gain,
        route_ids,
        route_weights,
        gate_weight,
        up_weight,
        down_weight,
    )


def fits_dense(mesh):
    ep_count, tp_count = mesh.shape["ep"], mesh.shape["tp"]
    return ep_count == 4 and tp_count >= 2 and tp_count & (tp_count - 1) == 0


def solution(mesh):
    dense = fits_dense(mesh)
    return jax.shard_map(
        shards_dense if dense else shards,
        mesh=mesh,
        in_specs=(
            P(("grp", "ep"), "tp"),
            P(("grp", "ep"), "tp"),
            P(("grp", "ep"), "tp"),
            P("tp", "ep"),
            P("tp", None),
            P(("grp", "ep"), None),
            P(),
            P(("grp", "ep"), None),
            P(("grp", "ep"), None),
            P("ep", None, "tp"),
            P("ep", None, "tp"),
            P("ep", "tp", None),
        ),
        out_specs=(P(("grp", "ep", "tp"), None), P(("grp", "ep", "tp"), None)),
        check_vma=False,
    )
```
